32 devices in a mesh: grp: 2 (over y), sp: 4 (over z), tp: 4 (over x, core).
Axes of the slice: x: 2, y: 2, z: 4, core: 2. Of those that a mesh axis runs over, the one named last changes fastest.
Arguments:
- residual: bfloat16 [2048, 2048], P(('grp', 'sp')), parts along dimension 0, may hold values from -34 to 34
- queries: bfloat16 [2048, 1024], P(('grp', 'sp'), 'tp'), parts along dimension 0, may hold values from -400 to 400
- keys: bfloat16 [2048, 512], P(('grp', 'sp'), 'tp'), parts along dimension 0, may hold values from -8 to 8
- values: bfloat16 [2048, 512], P(('grp', 'sp'), 'tp'), parts along dimension 0, may hold values from -6 to 6
- segments: int32 [2048], P(('grp', 'sp')), parts along dimension 0, may hold values from 0 to 2, never falling along the last dimension, each value on 1 to 768 neighbouring positions
- routes: int32 [2048, 2], P(('grp', 'sp')), parts along dimension 0, may hold values from 0 to 3, all different within a row; in each aligned block of 256 rows (0 to 255, 256 to 511, ...) at most 256 rows name the same one
- route_weight: float32 [2048, 2], P(('grp', 'sp')), parts along dimension 0, may hold values from 0.3 to 3
- sinks: float32 [16], P('tp'), may hold values from 1 to 6
- out_weight: bfloat16 [1024, 2048], P('tp'), may hold values from -1 to 1
- norm_gain: float32 [2048], replicated, may hold values from 0.1 to 1.9
- expert_gate: bfloat16 [4, 2048, 1024], P('sp', None, 'tp'), may hold values from -0.125 to 0.125
- expert_up: bfloat16 [4, 2048, 1024], P('sp', None, 'tp'), may hold values from -0.125 to 0.125
- expert_down: bfloat16 [4, 1024, 2048], P('sp', None, 'tp'), may hold values from -0.1875 to 0.1875
- shared_gate: bfloat16 [2048, 1024], P(None, 'tp'), may hold values from -0.125 to 0.125
- shared_up: bfloat16 [2048, 1024], P(None, 'tp'), may hold values from -0.125 to 0.125
- shared_down: bfloat16 [1024, 2048], P(None, 'tp'), may hold values from -0.1875 to 0.1875
Outputs:
- mixed: bfloat16 [2048, 2048], P(('grp', 'sp'), 'tp'), parts along dimension 0
The draws below stay inside these ranges and needn't reach their ends.
There are 2 independent parts, one for each index of `grp`. The reference program is written for one: setup_inputs(seed, part) draws one part's arguments, and reference() takes and returns one part's arrays. A program takes and returns all parts, laid end to end along the dimension named above; an argument that names none is the same for every part. Nothing has to cross between parts.
Inputs may be any that keep to these rules, and one draw needn't show every extreme that they name: `routes`: each row names 2 different experts. In the rows of one device no expert is named by more than 256 rows, and in some device's rows an expert is named by exactly 256. `segments`: document numbers never fall along the positions; every document spans 1 to 768 positions and one spans exactly 768.
All inputs are finite; a program needn't handle non-finite values.
Results may differ from the reference program's by a relative error of at most 0.0065.
Values may be sent and summed in bfloat16 or wider, within the bound.
No kernel may reach another device: no remote copies, remote signals or barrier semaphores. Data moves between devices by JAX's collectives and lax.ppermute only.
A program may use at most 64 MiB of HBM per device.

```python
import math
import jax
import jax.numpy as jnp
import numpy as np
from jax import lax

D = 2048
HEADS = 16
KV_HEADS = 8
HEAD_DIM = 64
WINDOW = 128
EFF = 1024
SFF = 1024
TOPK = 2
TOK = 256
TOKENS = 1024
EXPERTS = 4
CAP = 256
DOCS = 3
LONGEST = 768
N_SP = 4


def query_key_pair(key):
    query_seed = jax.random.fold_in(key, 101)
    key_seed = jax.random.fold_in(key, 202)
    queries = jnp.clip(jax.random.normal(query_seed, (TOKENS, HEADS * HEAD_DIM), jnp.float32), -6.0, 6.0)
    key_rows = jnp.clip(jax.random.normal(key_seed, (TOKENS, KV_HEADS * HEAD_DIM), jnp.float32), -6.0, 6.0)
    return (queries, key_rows)


def draw_queries(key, part):
    queries, key_rows = query_key_pair(key)
    return queries.astype(jnp.bfloat16)


def draw_keys(key, part):
    queries, key_rows = query_key_pair(key)
    return key_rows.astype(jnp.bfloat16)


def draw_residual(key, part):
    profile = jnp.exp(math.log(4.0) * jnp.arange(D, dtype=jnp.float32) / D)
    jitter = jnp.exp(jax.random.uniform(jax.random.fold_in(key, 11), (D,), jnp.float32, math.log(0.7), math.log(1.4)))
    base = jnp.clip(jax.random.normal(jax.random.fold_in(key, 14), (TOKENS, D), jnp.float32), -6.0, 6.0)
    return (base * profile * jitter).astype(jnp.bfloat16)


def level_of(own_key, shape, pieces, low, high):
    def one(dim, parts):
        heights = jax.random.uniform(jax.random.fold_in(jax.random.fold_in(own_key, 6), dim), (parts,), jnp.float32, low / len(pieces), high / len(pieces))
        return jnp.repeat(jnp.exp(heights), shape[dim] // parts).reshape((-1,) + (1,) * (len(shape) - dim - 1))

    factor_of = one(*pieces[0])
    for cut in pieces[1:]:
        factor_of = factor_of * one(*cut)
    return factor_of


def length_profile(amount, total, limit, skew):
    portions = [(1 << 20) // math.isqrt(grade ** skew) + 1 for grade in range(2, amount + 1)]
    rest, counts = total - limit - (amount - 1), [1] * (amount - 1)
    while rest > 0:
        movable = [i for i in range(amount - 1) if counts[i] < limit]
        whole, left = sum([portions[i] for i in movable]), rest
        for i in movable:
            addition = min(limit - counts[i], max(1, left * portions[i] // whole), rest)
            counts[i] = counts[i] + addition
            rest = rest - addition
    return np.array([limit] + counts)


def ragged(stream_key, count, total, reach, slope):
    if count == 2:
        one = jax.random.randint(stream_key, (), max(1, total - reach), min(reach, total - 1) + 1)
        return jnp.stack([one, total - one])
    sizes = jnp.asarray(length_profile(count, total, reach, slope), jnp.int32)
    twos = (count - 1) // 2
    source_of, taker = sizes[1:1 + 2 * twos:2], sizes[2:2 + 2 * twos:2]
    room = jnp.minimum(source_of - 1, reach - taker)
    passed = jax.random.randint(jax.random.fold_in(stream_key, 1), (twos,), 0, 1 << 20) % (room + 1)
    sizes = sizes.at[1:1 + 2 * twos:2].set(source_of - passed).at[2:2 + 2 * twos:2].set(taker + passed)
    return sizes[jax.random.permutation(jax.random.fold_in(stream_key, 2), count)]


def deal_out(key, own, number, rows, count, top, reach, lean):
    order = jax.random.permutation(key, count)
    heavy_load, usual = shares(count, rows * top, reach, lean, True), shares(count, rows * top, reach, lean, False)
    places = jnp.arange(count)

    def named(tallies, turn):
        used = int((tallies > 0).sum())
        fixed = max(1, used // 4)
        shifted = fixed + (places - fixed + turn * (used - fixed)) % max(1, count - fixed)
        return jnp.zeros((count,), jnp.int32).at[order[jnp.where(places < fixed, places, shifted)]].set(jnp.asarray(tallies, jnp.int32))

    tallies = jnp.where(number % 4 == 0, named(heavy_load, number // 4), named(usual, number - number // 4 - 1))
    mixed = jax.random.permutation(jax.random.fold_in(own, 3), count)
    source_of, taker = mixed[0:count // 2 * 2:2], mixed[1:count // 2 * 2:2]
    margin = jnp.minimum(tallies[source_of] - 1, reach - tallies[taker]) // 2
    margin = jnp.where((source_of == order[0]) | (taker == order[0]) | (tallies[taker] == 0), 0, jnp.maximum(margin, 0))
    shifted = jax.random.randint(jax.random.fold_in(own, 4), (count // 2,), 0, 1 << 20) % (margin + 1)
    tallies = tallies.at[source_of].add(-shifted).at[taker].add(shifted)
    members = jnp.searchsorted(jnp.cumsum(tallies), jnp.arange(rows * top), side="right").astype(jnp.int32)
    listing = members.reshape(top, rows).T
    listing = listing[jax.random.permutation(jax.random.fold_in(own, 1), rows)]
    turn = jax.random.randint(jax.random.fold_in(own, 2), (rows, 1), 0, top)
    return jnp.take_along_axis(listing, (jnp.arange(top)[None, :] + turn) % top, axis=1)


def shares(number_of, total, limit, skew, full):
    loads = [(1 << 20) // math.isqrt(grade ** skew) + 1 for grade in range(1, number_of + 1)]
    largest = limit if full else min(limit, max(-(-total // number_of), total * loads[0] // sum(loads)))
    least = 1 if total - largest >= number_of - 1 else 0
    counts, surplus = [largest] + [least] * (number_of - 1), total - largest - least * (number_of - 1)
    while surplus > 0:
        free = [i for i in range(1, number_of) if counts[i] < largest] or [i for i in range(1, number_of) if counts[i] < limit]
        mass, remaining = sum([loads[i] for i in free]), surplus
        for i in free:
            more = min(limit - counts[i], max(1, remaining * loads[i] // mass), surplus)
            counts[i] = counts[i] + more
            surplus = surplus - more
    return np.array(counts)


def centred(rng, extent, deviation, most, pieces=(), kind=jnp.bfloat16):
    array = jax.random.normal(rng, extent, jnp.float32) * deviation
    if len(pieces) > 0:
        array = level_of(rng, extent, pieces, -0.22, 0.18) * array
    return jnp.clip(array, min=-most, max=most).astype(kind)


def setup_inputs(seed: int = 0, part: int = 0) -> dict:
    key_of = jax.random.split(jax.random.key(seed), 17)
    part_keys = jax.random.split(jax.random.fold_in(key_of[16], part), 17)
    residual = draw_residual(jax.random.fold_in(jax.random.fold_in(key_of[16], part), 71), part)
    queries = draw_queries(jax.random.fold_in(jax.random.fold_in(key_of[16], part), 71), part)
    keys = draw_keys(jax.random.fold_in(jax.random.fold_in(key_of[16], part), 71), part)
    values = centred(part_keys[3], (TOKENS, KV_HEADS * HEAD_DIM), 1.0, 6.0, ((0, 4), (1, 4)))
    segments = jnp.searchsorted(jnp.cumsum(ragged(part_keys[4], DOCS, TOKENS, LONGEST, 2)), jnp.arange(TOKENS), side="right").astype(jnp.int32)
    routes_keys = jax.random.split(jax.random.fold_in(part_keys[5], 1), TOKENS // TOK)
    routes_turns = jax.random.permutation(jax.random.fold_in(part_keys[5], 3), TOKENS // TOK)
    routes = jax.vmap(lambda own, number: deal_out(jax.random.fold_in(part_keys[5], 2), own, number, TOK, EXPERTS, TOPK, CAP, 1))(routes_keys, routes_turns).reshape((TOKENS, TOPK))
    route_weight = jnp.clip(jnp.exp(math.log(3.0) - 2.3025851 * jax.random.uniform(part_keys[6], (TOKENS, TOPK), jnp.float32) ** level_of(part_keys[6], (TOKENS, TOPK), ((0, 4),), -0.2, 0.2)), 0.3, 3.0)
    sinks = jnp.clip(1.0 + 5.0 * jax.random.uniform(key_of[7], (HEADS,), jnp.float32) ** level_of(key_of[7], (HEADS,), ((0, 4),), -0.2, 0.2), 1.0, 6.0)
    out_weight = centred(key_of[8], (HEADS * HEAD_DIM, D), (HEADS * HEAD_DIM // 32) ** -0.5, 1.0, ((0, 4),))
    norm_gain = jnp.clip(1.0 + 0.18 * jax.random.normal(key_of[9], (D,), jnp.float32), 0.1, 1.9)
    expert_gate = centred(key_of[10], (EXPERTS, D, EFF), D ** -0.5, 0.125, ((0, 4), (2, 4)))
    expert_up = centred(key_of[11], (EXPERTS, D, EFF), D ** -0.5, 0.125, ((0, 4), (2, 4)))
    expert_down = centred(key_of[12], (EXPERTS, EFF, D), EFF ** -0.5, 0.1875, ((0, 4), (2, 4)))
    shared_gate = centred(key_of[13], (D, SFF), D ** -0.5, 0.125, ((1, 4),))
    shared_up = centred(key_of[14], (D, SFF), D ** -0.5, 0.125, ((1, 4),))
    shared_down = centred(key_of[15], (SFF, D), SFF ** -0.5, 0.1875, ((1, 4),))
    return {"residual": residual, "queries": queries, "keys": keys, "values": values, "segments": segments, "routes": routes, "route_weight": route_weight, "sinks": sinks, "out_weight": out_weight, "norm_gain": norm_gain, "expert_gate": expert_gate, "expert_up": expert_up, "expert_down": expert_down, "shared_gate": shared_gate, "shared_up": shared_up, "shared_down": shared_down}


epsilon = 1e-06

def banded(rows, fill):
    blocks = rows.shape[0] // WINDOW
    shaped = rows.reshape((blocks, WINDOW) + rows.shape[1:])
    before = jnp.concatenate([jnp.full_like(shaped[:1], fill), shaped[:-1]], axis=0)
    return jnp.concatenate([before, shaped], axis=1)

def attend(queries, keys, values, segments, sinks):
    blocks = TOKENS // WINDOW
    group_size = HEADS // KV_HEADS
    query_blocks = queries.astype(jnp.float32).reshape(blocks, WINDOW, KV_HEADS, group_size, HEAD_DIM)
    key_band = banded(keys, 0).astype(jnp.float32).reshape(blocks, 2 * WINDOW, KV_HEADS, HEAD_DIM)
    value_band = banded(values, 0).astype(jnp.float32).reshape(blocks, 2 * WINDOW, KV_HEADS, HEAD_DIM)
    segment_band = banded(segments, -1)
    query_segments = segments.reshape(blocks, WINDOW)
    scores = jnp.einsum('nqhgd,nkhd->nhgqk', query_blocks, key_band) * HEAD_DIM ** (-0.5)
    offsets = jnp.arange(WINDOW)[:, None] + WINDOW - jnp.arange(2 * WINDOW)[None, :]
    allowed = (offsets >= 0) & (offsets < WINDOW) & (query_segments[:, :, None] == segment_band[:, None, :])
    sink_logits = sinks.astype(jnp.float32).reshape(KV_HEADS, group_size)[None, :, :, None]
    masked = jnp.where(allowed[:, None, None], scores, -jnp.inf)
    top_score = jnp.maximum(lax.optimization_barrier(jnp.max(masked, axis=-1)), sink_logits)
    exp_terms = jnp.where(allowed[:, None, None], jnp.exp(scores - top_score[..., None]), 0.0)
    denominator = lax.optimization_barrier(jnp.sum(exp_terms, axis=-1)) + jnp.exp(sink_logits - top_score)
    probabilities = (exp_terms / denominator[..., None]).astype(jnp.bfloat16)
    attended = jnp.einsum('nhgqk,nkhd->nqhgd', probabilities.astype(jnp.float32), value_band)
    return attended.astype(jnp.bfloat16).reshape(TOKENS, HEADS * HEAD_DIM)

def block_slots(block_routes):
    flat_ids = block_routes.reshape(-1)
    one_hot = (flat_ids[:, None] == jnp.arange(EXPERTS, dtype=jnp.int32)[None, :]).astype(jnp.int32)
    rank_in = jnp.cumsum(one_hot, axis=0) - one_hot
    return flat_ids * CAP + lax.optimization_barrier(jnp.sum(rank_in * one_hot, axis=1))

def reference(residual, queries, keys, values, segments, routes, route_weight, sinks, out_weight, norm_gain, expert_gate, expert_up, expert_down, shared_gate, shared_up, shared_down):
    attended = attend(queries, keys, values, segments, sinks)
    projected = jnp.dot(attended, out_weight, preferred_element_type=jnp.float32)
    updated = (residual.astype(jnp.float32) + projected).astype(jnp.bfloat16)
    updated_f32 = updated.astype(jnp.float32)
    inv_rms = lax.rsqrt(lax.optimization_barrier(jnp.mean(updated_f32 * updated_f32, axis=-1, keepdims=True)) + epsilon)
    normed = (updated_f32 * inv_rms * norm_gain).astype(jnp.bfloat16)
    shared_pre = jnp.dot(normed, shared_gate, preferred_element_type=jnp.float32)
    shared_lin = jnp.dot(normed, shared_up, preferred_element_type=jnp.float32)
    shared_act = (jax.nn.silu(shared_pre) * shared_lin).astype(jnp.bfloat16)
    shared_out = jnp.dot(shared_act, shared_down, preferred_element_type=jnp.float32)
    slot_dest = jax.vmap(block_slots)(routes.reshape(N_SP, TOK, TOPK))
    block_ids = jnp.broadcast_to(jnp.arange(N_SP, dtype=jnp.int32)[:, None], slot_dest.shape)
    token_ids = block_ids * TOK + (jnp.arange(TOK * TOPK, dtype=jnp.int32) // TOPK)[None, :]
    slot_token = jnp.full((N_SP, EXPERTS * CAP), -1, jnp.int32).at[block_ids, slot_dest].set(token_ids)
    slot_weight = jnp.zeros((N_SP, EXPERTS * CAP), jnp.float32).at[block_ids, slot_dest].set(route_weight.reshape(N_SP, TOK * TOPK))
    per_token = slot_token.reshape(N_SP, EXPERTS, CAP).transpose(1, 0, 2).reshape(EXPERTS, N_SP * CAP)
    per_weight = slot_weight.reshape(N_SP, EXPERTS, CAP).transpose(1, 0, 2).reshape(EXPERTS, N_SP * CAP)

    def one_expert(accum, inputs):
        gate_mat, up_mat, down_mat, token_list, weight_list = inputs
        filled = token_list >= 0
        safe_token = jnp.where(filled, token_list, 0).astype(jnp.int32)
        rows_in = jnp.where(filled[:, None], normed[safe_token], jnp.zeros((), jnp.bfloat16))
        gate_pre = jnp.dot(rows_in, gate_mat, preferred_element_type=jnp.float32)
        up_lin = jnp.dot(rows_in, up_mat, preferred_element_type=jnp.float32)
        expert_act = (jax.nn.silu(gate_pre) * up_lin).astype(jnp.bfloat16)
        expert_out = jnp.dot(expert_act, down_mat, preferred_element_type=jnp.float32).astype(jnp.bfloat16)
        accum = accum.at[safe_token].add(expert_out.astype(jnp.float32) * weight_list[:, None])
        return (accum, None)
    routed, _ = lax.scan(one_expert, jnp.zeros((TOKENS, D), jnp.float32), (expert_gate, expert_up, expert_down, per_token, per_weight))
    return (updated_f32 + shared_out + routed).astype(jnp.bfloat16)
```

```python
import functools

import jax
import jax.numpy as jnp
from jax import lax
from jax.experimental import pallas as pl
from jax.experimental.pallas import tpu as pltpu
from jax.sharding import PartitionSpec as P

HEAD_DIM = 64
WINDOW = 128


epsilon = 1e-06


def passed_along(value, axis, steps):
    count = lax.axis_size(axis)
    leading, last = (max(0, -steps), min(count, count - steps))
    return lax.ppermute(value, axis, [(source, source + steps) for source in range(leading, last)])


def banded(prev_rows, own_rows, window_len):
    blocks = own_rows.shape[0] // window_len
    joined = jnp.concatenate([prev_rows, own_rows], axis=0)
    shaped = joined.reshape((blocks + 1, window_len) + own_rows.shape[1:])
    return jnp.concatenate([shaped[:-1], shaped[1:]], axis=1)


def swapped(value, axis, bit):
    count = lax.axis_size(axis)
    return lax.ppermute(value, axis, [(source, source ^ bit) for source in range(count)])


def gathered(value, axis):
    pieces = {0: value}
    bit = lax.axis_size(axis) // 2
    while bit:
        pieces.update({known ^ bit: swapped(held, axis, bit) for known, held in pieces.items()})
        bit //= 2
    return [pieces[j] for j in range(len(pieces))]


def dot32(left, right):
    return jnp.dot(left, right, preferred_element_type=jnp.float32)


def attend_kernel(sink_ref, q_ref, k_ref, v_ref, halo_ref, col_ref, row_ref, out_ref):
    span = WINDOW
    rows = q_ref.shape[0]
    kv_local = k_ref.shape[1] // HEAD_DIM
    group_size = q_ref.shape[1] // k_ref.shape[1]
    halo = halo_ref[...]
    keys = jnp.concatenate([halo[:span], k_ref[...]], axis=0)
    values = jnp.concatenate([halo[span : 2 * span], v_ref[...]], axis=0)
    marks = jnp.concatenate([halo[2 * span : 2 * span + 1].astype(jnp.float32), row_ref[...]], axis=1)
    place = lax.broadcasted_iota(jnp.int32, (span, 2 * span), 0)
    offsets = place + span - lax.broadcasted_iota(jnp.int32, (span, 2 * span), 1)
    near = (offsets >= 0) & (offsets < span)
    for block in range(rows // span):
        low = block * span
        allowed = near & (col_ref[low : low + span, :] == marks[:, low : low + 2 * span])
        outs = []
        for kv in range(kv_local):
            lanes = slice(kv * HEAD_DIM, (kv + 1) * HEAD_DIM)
            key_part = keys[low : low + 2 * span, lanes]
            value_part = values[low : low + 2 * span, lanes]
            for member in range(group_size):
                head = kv * group_size + member
                query = q_ref[low : low + span, head * HEAD_DIM : (head + 1) * HEAD_DIM]
                scores = lax.dot_general(
                    query, key_part, (((1,), (1,)), ((), ())), preferred_element_type=jnp.float32
                ) * HEAD_DIM ** (-0.5)
                sink = sink_ref[head]
                masked = jnp.where(allowed, scores, -jnp.inf)
                top = jnp.maximum(jnp.max(masked, axis=1, keepdims=True), sink)
                terms = jnp.exp(masked - top)
                total = jnp.sum(terms, axis=1, keepdims=True) + jnp.exp(sink - top)
                probs = (terms / total).astype(jnp.bfloat16)
                outs.append(dot32(probs, value_part).astype(jnp.bfloat16))
        out_ref[low : low + span, :] = jnp.concatenate(outs, axis=1)


def update_kernel(count, residual_ref, *refs):
    total = residual_ref[...].astype(jnp.float32)
    for j in range(count):
        total = total + dot32(refs[j][...], refs[count + j][...])
    refs[-1][...] = total.astype(jnp.bfloat16)


def hidden_kernel(count, pairs, place_ref, gain_ref, *refs):
    pieces = [ref[...].astype(jnp.float32) for ref in refs[:count]]
    weights = refs[count : count + 2 * pairs]
    outs = refs[count + 2 * pairs :]
    width = sum(piece.shape[1] for piece in pieces)
    squares = sum(jnp.sum(piece * piece, axis=1, keepdims=True) for piece in pieces)
    scale = lax.rsqrt(squares / width + epsilon)
    place = place_ref[0]
    sums = [None] * (2 * pairs)
    for j in range(count):
        at = place ^ j
        normed = (pieces[j] * scale * gain_ref[at]).astype(jnp.bfloat16)
        for n in range(2 * pairs):
            term = dot32(normed, weights[n][at])
            sums[n] = term if j == 0 else sums[n] + term
    for n in range(pairs):
        gate, lin = sums[2 * n], sums[2 * n + 1]
        outs[n][...] = (gate / (1.0 + jnp.exp(-gate)) * lin).astype(jnp.bfloat16)


def down_kernel(count, place_ref, down_ref, *refs):
    place = place_ref[0]
    total = dot32(refs[0][...], down_ref[place])
    for j in range(1, count):
        total = total + dot32(refs[j][...], down_ref[place ^ j])
    refs[-1][...] = total.astype(jnp.bfloat16)


def own_kernel(count, place_ref, down_ref, shared_ref, updated_ref, weight_ref, *refs):
    place = place_ref[0]
    routed = dot32(refs[0][...], down_ref[place])
    common = dot32(refs[count][...], shared_ref[place])
    for j in range(1, count):
        routed = routed + dot32(refs[j][...], down_ref[place ^ j])
        common = common + dot32(refs[count + j][...], shared_ref[place ^ j])
    routed = routed.astype(jnp.bfloat16).astype(jnp.float32)
    refs[-1][...] = updated_ref[...].astype(jnp.float32) + common + routed * weight_ref[...]


def mix_kernel(count, base_ref, *refs):
    total = base_ref[...]
    for k in range(count):
        total = total + refs[k][...].astype(jnp.float32) * refs[count + k][...]
    refs[-1][...] = total.astype(jnp.bfloat16)


def call(kernel, out, args, scalars=0, name=None):
    specs = [pl.BlockSpec(memory_space=pltpu.SMEM if n < scalars else pltpu.VMEM) for n in range(len(args))]
    vmem = pl.BlockSpec(memory_space=pltpu.VMEM)
    several = isinstance(out, list)
    return pl.pallas_call(
        kernel, out_shape=out, in_specs=specs, out_specs=[vmem] * len(out) if several else vmem, name=name
    )(*args)


def dense_shards(
    residual,
    queries,
    keys,
    values,
    segments,
    routes,
    route_weight,
    sinks,
    out_weight,
    norm_gain,
    expert_gate,
    expert_up,
    expert_down,
    shared_gate,
    shared_up,
    shared_down,
):
    rows_here, model_width = residual.shape
    tp_count, sp_count = lax.axis_size("tp"), lax.axis_size("sp")
    tp_index, sp_index = lax.axis_index("tp"), lax.axis_index("sp")
    place = tp_index.astype(jnp.int32).reshape(1)
    span = WINDOW
    col_width = model_width // tp_count
    bf16 = jnp.bfloat16

    own_marks = (segments % 256 + 1).astype(jnp.float32)
    packed = jnp.concatenate(
        [
            keys[rows_here - span :],
            values[rows_here - span :],
            jnp.broadcast_to(own_marks[rows_here - span :].astype(bf16)[None, :], (16, span)),
        ],
        axis=0,
    )
    halo = passed_along(packed, "sp", 1)

    out_parts = []
    for j in range(tp_count):
        part = lax.dynamic_slice_in_dim(out_weight, (tp_index ^ j) * col_width, col_width, 1)
        out_parts.append(part if j == 0 else swapped(part, "tp", j))

    attended = call(
        attend_kernel,
        jax.ShapeDtypeStruct(queries.shape, bf16),
        [sinks, queries, keys, values, halo, own_marks[:, None], own_marks[None, :]],
        1,
        "attend",
    )
    residual_cols = lax.dynamic_slice_in_dim(residual, tp_index * col_width, col_width, 1)
    own = call(
        functools.partial(update_kernel, tp_count),
        jax.ShapeDtypeStruct((rows_here, col_width), bf16),
        [residual_cols, *gathered(attended, "tp"), *out_parts],
        0,
        "update",
    )

    gain = norm_gain.reshape(tp_count, 1, col_width)
    gate = expert_gate.reshape(tp_count, col_width, -1)
    up = expert_up.reshape(tp_count, col_width, -1)
    shared_gate = shared_gate.reshape(tp_count, col_width, -1)
    shared_up = shared_up.reshape(tp_count, col_width, -1)
    hidden = gate.shape[2]
    shared_hidden = shared_gate.shape[2]
    down = expert_down.reshape(tp_count, hidden, col_width)
    shared_down = shared_down.reshape(tp_count, shared_hidden, col_width)
    act_shape = jax.ShapeDtypeStruct((rows_here, hidden), bf16)
    shared_shape = jax.ShapeDtypeStruct((rows_here, shared_hidden), bf16)

    def weight_of(step):
        named = routes == (sp_index ^ step)
        return jnp.sum(jnp.where(named, route_weight, 0.0), axis=1, keepdims=True)

    blocks = [own] + [swapped(own, "sp", k) for k in range(1, sp_count)]
    returned = []
    base = None
    for k in range(sp_count):
        pieces = gathered(blocks[k], "tp")
        if k == 0:
            act, shared_act = call(
                functools.partial(hidden_kernel, tp_count, 2),
                [act_shape, shared_shape],
                [place, gain, *pieces, gate, up, shared_gate, shared_up],
                1,
                "hidden_own",
            )
            base = call(
                functools.partial(own_kernel, tp_count),
                jax.ShapeDtypeStruct((rows_here, col_width), jnp.float32),
                [place, down, shared_down, own, weight_of(0), *gathered(act, "tp"), *gathered(shared_act, "tp")],
                1,
                "down_own",
            )
        else:
            (act,) = call(
                functools.partial(hidden_kernel, tp_count, 1),
                [act_shape],
                [place, gain, *pieces, gate, up],
                1,
                "hidden",
            )
            out = call(
                functools.partial(down_kernel, tp_count),
                jax.ShapeDtypeStruct((rows_here, col_width), bf16),
                [place, down, *gathered(act, "tp")],
                1,
                "down",
            )
            returned.append(swapped(out, "sp", k))
    return call(
        functools.partial(mix_kernel, sp_count - 1),
        jax.ShapeDtypeStruct((rows_here, col_width), bf16),
        [base, *returned, *[weight_of(k) for k in range(1, sp_count)]],
        0,
        "mix",
    )


def shards(
    residual,
    queries,
    keys,
    values,
    segments,
    routes,
    route_weight,
    sinks,
    out_weight,
    norm_gain,
    expert_gate,
    expert_up,
    expert_down,
    shared_gate,
    shared_up,
    shared_down,
):
    rows_here = residual.shape[0]
    model_width = residual.shape[1]
    tp_count = lax.axis_size("tp")
    tp_index = lax.axis_index("tp")
    head_local = queries.shape[1] // HEAD_DIM
    kv_local = keys.shape[1] // HEAD_DIM
    group_size = head_local // kv_local
    window_len = WINDOW
    blocks = rows_here // window_len
    own_marks = (segments % 256 + 1).astype(jnp.bfloat16)
    prev_keys, prev_values, prev_marks = passed_along(
        (
            keys[rows_here - window_len :],
            values[rows_here - window_len :],
            own_marks[rows_here - window_len :],
        ),
        "sp",
        1,
    )
    key_band = banded(prev_keys, keys, window_len).reshape(
        blocks, 2 * window_len, kv_local, HEAD_DIM
    )
    value_band = banded(prev_values, values, window_len).reshape(
        blocks, 2 * window_len, kv_local, HEAD_DIM
    )
    mark_band = banded(prev_marks, own_marks, window_len).astype(jnp.float32)
    query_marks = own_marks.reshape(blocks, window_len).astype(jnp.float32)
    query_blocks = queries.reshape(blocks, window_len, kv_local, group_size, HEAD_DIM)
    scores = jnp.einsum(
        "nqhgd,nkhd->nhgqk", query_blocks, key_band, preferred_element_type=jnp.float32
    ) * HEAD_DIM ** (-0.5)
    offsets = jnp.arange(window_len)[:, None] + window_len - jnp.arange(2 * window_len)[None, :]
    allowed = (
        (offsets >= 0) & (offsets < window_len) & (query_marks[:, :, None] == mark_band[:, None, :])
    )
    sink_logits = sinks.reshape(kv_local, group_size)[None, :, :, None]
    masked = jnp.where(allowed[:, None, None], scores, -jnp.inf)
    top_score = jnp.maximum(jnp.max(masked, axis=-1), sink_logits)
    exp_terms = jnp.where(allowed[:, None, None], jnp.exp(scores - top_score[..., None]), 0.0)
    denominator = jnp.sum(exp_terms, axis=-1) + jnp.exp(sink_logits - top_score)
    probabilities = (exp_terms / denominator[..., None]).astype(jnp.bfloat16)
    attended = jnp.einsum(
        "nhgqk,nkhd->nqhgd", probabilities, value_band, preferred_element_type=jnp.float32
    )
    attended = attended.astype(jnp.bfloat16).reshape(rows_here, head_local * HEAD_DIM)
    partial_value = jnp.dot(attended, out_weight, preferred_element_type=jnp.float32)
    col_width = model_width // tp_count
    col_start = tp_index * col_width
    summed = lax.psum(partial_value, "tp")
    updated = (residual.astype(jnp.float32) + summed).astype(jnp.bfloat16)
    updated_f32 = updated.astype(jnp.float32)
    inv_rms = lax.rsqrt(jnp.mean(updated_f32 * updated_f32, axis=-1, keepdims=True) + epsilon)
    normed = (updated_f32 * inv_rms * norm_gain).astype(jnp.bfloat16)
    updated_cols = lax.dynamic_slice_in_dim(updated, col_start, col_width, 1)
    normed_cols = lax.dynamic_slice_in_dim(normed, col_start, col_width, 1)
    shared_pre = jnp.dot(normed, shared_gate, preferred_element_type=jnp.float32)
    shared_lin = jnp.dot(normed, shared_up, preferred_element_type=jnp.float32)
    shared_act = (jax.nn.silu(shared_pre) * shared_lin).astype(jnp.bfloat16)
    top_count = routes.shape[1]
    experts = lax.axis_size("sp")
    capacity = 2 * rows_here * top_count // experts
    flat_ids = routes.reshape(-1)
    one_hot = (flat_ids[:, None] == jnp.arange(experts, dtype=jnp.int32)[None, :]).astype(jnp.int32)
    rank_in = jnp.cumsum(one_hot, axis=0) - one_hot
    slot_dest = flat_ids * capacity + jnp.sum(rank_in * one_hot, axis=1)
    token_of = jnp.arange(rows_here * top_count, dtype=jnp.int32) // top_count
    slot_token = jnp.full((experts * capacity,), -1, jnp.int32).at[slot_dest].set(token_of)
    filled = slot_token >= 0
    safe_token = jnp.where(filled, slot_token, 0)
    outgoing = jnp.where(filled[:, None], normed_cols[safe_token], jnp.zeros((), jnp.bfloat16))
    pieces = lax.all_to_all(
        outgoing.reshape(experts, capacity, col_width),
        "sp",
        split_axis=0,
        concat_axis=0,
        tiled=True,
    )
    arrived = lax.all_gather(pieces, "tp", axis=2, tiled=True)
    expert_rows = arrived.reshape(-1, model_width)
    gate_pre = jnp.dot(expert_rows, expert_gate[0], preferred_element_type=jnp.float32)
    up_lin = jnp.dot(expert_rows, expert_up[0], preferred_element_type=jnp.float32)
    expert_act = (jax.nn.silu(gate_pre) * up_lin).astype(jnp.bfloat16)
    gathered_expert, gathered_shared = (
        lax.all_gather(expert_act, "tp", axis=1, tiled=True),
        lax.all_gather(shared_act, "tp", axis=1, tiled=True),
    )
    expert_out = jnp.dot(
        gathered_expert, expert_down[0], preferred_element_type=jnp.float32
    ).astype(jnp.bfloat16)
    returned = lax.all_to_all(
        expert_out.reshape(experts, capacity, col_width),
        "sp",
        split_axis=0,
        concat_axis=0,
        tiled=True,
    )
    returned = returned.reshape(experts * capacity, col_width)
    picked = returned[slot_dest].astype(jnp.float32).reshape(rows_here, top_count, col_width)
    routed = jnp.sum(picked * route_weight[:, :, None], axis=1)
    shared_cols = jnp.dot(gathered_shared, shared_down, preferred_element_type=jnp.float32)
    return (updated_cols.astype(jnp.float32) + shared_cols + routed).astype(jnp.bfloat16)


def choose(*args):
    rows_here, model_width = args[0].shape
    experts, tp_count = lax.axis_size("sp"), lax.axis_size("tp")
    dense = 2 * rows_here * args[5].shape[1] // experts >= rows_here
    even = experts & (experts - 1) == 0 and tp_count & (tp_count - 1) == 0
    fits = args[2].shape[1] == WINDOW and rows_here % WINDOW == 0
    return (dense_shards if dense and even and fits else shards)(*args)


def solution(mesh):
    placed = (
        P(("grp", "sp"), None),
        P(("grp", "sp"), "tp"),
        P(("grp", "sp"), "tp"),
        P(("grp", "sp"), "tp"),
        P(("grp", "sp")),
        P(("grp", "sp"), None),
        P(("grp", "sp"), None),
        P("tp"),
        P("tp", None),
        P(),
        P("sp", None, "tp"),
        P("sp", None, "tp"),
        P("sp", None, "tp"),
        P(None, "tp"),
        P(None, "tp"),
        P(None, "tp"),
    )
    return jax.shard_map(
        choose, mesh=mesh, in_specs=placed, out_specs=P(("grp", "sp"), "tp"), check_vma=False
    )
```

```python
import functools

import jax
import jax.numpy as jnp
from jax import lax
from jax.experimental import pallas as pl
from jax.experimental.pallas import tpu as pltpu
from jax.sharding import PartitionSpec as P


HEAD_DIM = 64
WINDOW = 128


epsilon = 1e-06


def passed_along(value, axis, steps):
    count = lax.axis_size(axis)
    leading, last = (max(0, -steps), min(count, count - steps))
    return lax.ppermute(value, axis, [(source, source + steps) for source in range(leading, last)])


def banded(prev_rows, own_rows, window_len):
    blocks = own_rows.shape[0] // window_len
    joined = jnp.concatenate([prev_rows, own_rows], axis=0)
    shaped = joined.reshape((blocks + 1, window_len) + own_rows.shape[1:])
    return jnp.concatenate([shaped[:-1], shaped[1:]], axis=1)


KERNEL_VMEM = 16 * 2**20


def swapped(value, axis, bit):
    count = lax.axis_size(axis)
    return lax.ppermute(value, axis, [(source, source ^ bit) for source in range(count)])


def gathered(value):
    pieces = {0: value}
    bit = lax.axis_size("tp") // 2
    while bit:
        more = {}
        for known, held in pieces.items():
            more[known ^ bit] = swapped(held, "tp", bit)
        pieces.update(more)
        bit //= 2
    return [pieces[j] for j in range(len(pieces))]


def dot32(left, right):
    return jnp.dot(left, right, preferred_element_type=jnp.float32)


def columns(ref, spot):
    width = ref.shape[1] // lax.axis_size("tp")
    return ref[:, pl.ds(pl.multiple_of(spot * width, width), width)]


def column(row):
    return jnp.transpose(jnp.broadcast_to(row, (8, row.shape[1])))[:, :1]


def prologue_kernel(place_ref, marks_ref, k_ref, v_ref, out_ref, packed_ref, *part_refs):
    span, rows = WINDOW, k_ref.shape[0]
    tail = slice(rows - span, rows)
    packed_ref[:span, :] = k_ref[tail, :]
    packed_ref[span : 2 * span, :] = v_ref[tail, :]
    marks = jnp.broadcast_to(marks_ref[:, tail], (packed_ref.shape[0] - 2 * span, span))
    packed_ref[2 * span :, :] = marks.astype(jnp.bfloat16)
    for j, part_ref in enumerate(part_refs, 1):
        part_ref[...] = columns(out_ref, place_ref[0] ^ j)


def attend_kernel(sink_ref, row_ref, q_ref, k_ref, v_ref, halo_ref, out_ref):
    span = WINDOW
    rows = q_ref.shape[0]
    kv_local = k_ref.shape[1] // HEAD_DIM
    group_size = q_ref.shape[1] // k_ref.shape[1]
    halo = halo_ref[...]
    keys = jnp.concatenate([halo[:span], k_ref[...]], axis=0)
    values = jnp.concatenate([halo[span : 2 * span], v_ref[...]], axis=0)
    own = row_ref[...]
    marks = jnp.concatenate([halo[2 * span : 2 * span + 1].astype(jnp.float32), own], axis=1)
    down_marks = column(own)
    place = lax.broadcasted_iota(jnp.int32, (span, 2 * span), 0)
    offsets = place + span - lax.broadcasted_iota(jnp.int32, (span, 2 * span), 1)
    near = (offsets >= 0) & (offsets < span)
    for block in range(rows // span):
        low = block * span
        allowed = near & (down_marks[low : low + span] == marks[:, low : low + 2 * span])
        outs = []
        for kv in range(kv_local):
            lanes = slice(kv * HEAD_DIM, (kv + 1) * HEAD_DIM)
            key_part = keys[low : low + 2 * span, lanes]
            value_part = values[low : low + 2 * span, lanes]
            for member in range(group_size):
                head = kv * group_size + member
                query = q_ref[low : low + span, head * HEAD_DIM : (head + 1) * HEAD_DIM]
                scores = lax.dot_general(
                    query, key_part, (((1,), (1,)), ((), ())), preferred_element_type=jnp.float32
                ) * HEAD_DIM ** (-0.5)
                sink = sink_ref[head]
                masked = jnp.where(allowed, scores, -jnp.inf)
                top = jnp.maximum(jnp.max(masked, axis=1, keepdims=True), sink)
                terms = jnp.exp(masked - top)
                total = jnp.sum(terms, axis=1, keepdims=True) + jnp.exp(sink - top)
                probs = (terms / total).astype(jnp.bfloat16)
                outs.append(dot32(probs, value_part).astype(jnp.bfloat16))
        out_ref[low : low + span, :] = jnp.concatenate(outs, axis=1)


def update_kernel(count, place_ref, residual_ref, weight_ref, *refs):
    acts, parts, out_ref = refs[:count], refs[count:-1], refs[-1]
    place = place_ref[0]
    total = columns(residual_ref, place).astype(jnp.float32)
    total = total + dot32(acts[0][...], columns(weight_ref, place))
    for act, part in zip(acts[1:], parts, strict=True):
        total = total + dot32(act[...], part[...])
    out_ref[...] = total.astype(jnp.bfloat16)


def hidden_kernel(count, pairs, place_ref, gain_ref, *refs):
    pieces, weights, out_ref = refs[:count], refs[count:-1], refs[-1]
    place = place_ref[0]
    width = sum(piece.shape[1] for piece in pieces)
    hidden = weights[0].shape[2]
    squares = 0.0
    for piece in pieces:
        rows = piece[...].astype(jnp.float32)
        squares = squares + jnp.sum(rows * rows, axis=1, keepdims=True)
    scale = lax.rsqrt(squares / width + epsilon)
    sums = [None] * (2 * pairs)
    for j in range(count):
        at = place ^ j
        normed = (pieces[j][...].astype(jnp.float32) * scale * gain_ref[at]).astype(jnp.bfloat16)
        for n in range(2 * pairs):
            term = dot32(normed, weights[n][at])
            sums[n] = term if j == 0 else sums[n] + term
    for n in range(pairs):
        gate, lin = sums[2 * n], sums[2 * n + 1]
        act = gate / (1.0 + jnp.exp(-gate)) * lin
        out_ref[:, n * hidden : (n + 1) * hidden] = act.astype(jnp.bfloat16)


def down_kernel(count, place_ref, down_ref, *refs):
    place = place_ref[0]
    total = dot32(refs[0][...], down_ref[place])
    for j in range(1, count):
        total = total + dot32(refs[j][...], down_ref[place ^ j])
    refs[-1][...] = total.astype(jnp.bfloat16)


def weights_of(spot, routes_ref, weight_ref, steps):
    routes, weight = routes_ref[...], weight_ref[...]
    rows = []
    for k in range(steps):
        named = jnp.where(routes == (spot ^ k), weight, 0.0)
        rows.append(jnp.sum(named, axis=0, keepdims=True))
    rows += [jnp.zeros_like(rows[0])] * (-steps % 8)
    return jnp.transpose(jnp.concatenate(rows, axis=0))


def own_kernel(count, place_ref, routes_ref, weight_ref, down_ref, shared_ref, updated_ref, *refs):
    place = place_ref[0]
    hidden = down_ref.shape[1]
    for j in range(count):
        terms = [
            dot32(refs[j][:, :hidden], down_ref[place ^ j]),
            dot32(refs[j][:, hidden:], shared_ref[place ^ j]),
        ]
        sums = terms if j == 0 else [old + term for old, term in zip(sums, terms, strict=True)]
    weight = weights_of(place_ref[1], routes_ref, weight_ref, 1)[:, :1]
    routed = sums[0].astype(jnp.bfloat16).astype(jnp.float32)
    refs[-1][...] = updated_ref[...].astype(jnp.float32) + sums[1] + routed * weight


def mix_kernel(count, place_ref, routes_ref, weight_ref, base_ref, *refs):
    weights = weights_of(place_ref[1], routes_ref, weight_ref, count + 1)
    total = base_ref[...]
    for k in range(count):
        total = total + refs[k][...].astype(jnp.float32) * weights[:, k + 1 : k + 2]
    refs[-1][...] = total.astype(jnp.bfloat16)


def call(kernel, out, args, scalars=1):
    specs = [pl.BlockSpec(memory_space=pltpu.SMEM if n < scalars else pltpu.VMEM) for n in range(len(args))]
    vmem = pl.BlockSpec(memory_space=pltpu.VMEM)
    return pl.pallas_call(
        kernel,
        out_shape=out,
        in_specs=specs,
        out_specs=[vmem] * len(out) if isinstance(out, list) else vmem,
        compiler_params=pltpu.CompilerParams(vmem_limit_bytes=KERNEL_VMEM),
    )(*args)


def dense_shards(*args):
    return dense_steps(*args)


def dense_steps(
    residual,
    queries,
    keys,
    values,
    segments,
    routes,
    route_weight,
    sinks,
    out_weight,
    norm_gain,
    expert_gate,
    expert_up,
    expert_down,
    shared_gate,
    shared_up,
    shared_down,
):
    rows_here, model_width = residual.shape
    tp_count, sp_count = lax.axis_size("tp"), lax.axis_size("sp")
    tp_index = lax.axis_index("tp").astype(jnp.int32)
    sp_index = lax.axis_index("sp").astype(jnp.int32)
    place = jnp.stack([tp_index, sp_index])
    span = WINDOW
    col_width = model_width // tp_count
    heads_width = out_weight.shape[0]
    bf16, f32 = jnp.bfloat16, jnp.float32
    shape = jax.ShapeDtypeStruct

    own_marks = (segments % 256 + 1).astype(f32)[None, :]
    packed, *parts = call(
        prologue_kernel,
        [shape((2 * span + 16, span), bf16)] + [shape((heads_width, col_width), bf16)] * (tp_count - 1),
        [place, own_marks, keys, values, out_weight],
    )
    halo = passed_along(packed, "sp", 1)
    parts = [swapped(part, "tp", j) for j, part in enumerate(parts, 1)]
    attended = call(
        attend_kernel, shape(queries.shape, bf16), [sinks, own_marks, queries, keys, values, halo]
    )
    own = call(
        functools.partial(update_kernel, tp_count),
        shape((rows_here, col_width), bf16),
        [place, residual, out_weight, *gathered(attended), *parts],
    )

    gain = norm_gain.reshape(tp_count, 1, col_width)
    gate, up, common_gate, common_up = [
        weight.reshape(tp_count, col_width, -1) for weight in (expert_gate, expert_up, shared_gate, shared_up)
    ]
    hidden = gate.shape[2]
    down, common_down = [weight.reshape(tp_count, hidden, col_width) for weight in (expert_down, shared_down)]
    routes, route_weight = routes.T, route_weight.T
    cols = (rows_here, col_width)

    blocks = [own] + [swapped(own, "sp", k) for k in range(1, sp_count - 1)]
    blocks.append(swapped(blocks[(sp_count - 1) ^ 1], "sp", 1))
    returned = []
    base = None
    for k in range(sp_count):
        pieces = gathered(blocks[k])
        pairs = 2 if k == 0 else 1
        weights = [gate, up, common_gate, common_up][: 2 * pairs]
        act = call(
            functools.partial(hidden_kernel, tp_count, pairs),
            shape((rows_here, pairs * hidden), bf16),
            [place, gain, *pieces, *weights],
        )
        acts = gathered(act)
        if k == 0:
            base = call(
                functools.partial(own_kernel, tp_count),
                shape(cols, f32),
                [place, routes, route_weight, down, common_down, own, *acts],
            )
        else:
            out = call(
                functools.partial(down_kernel, tp_count), shape(cols, bf16), [place, down, *acts]
            )
            returned.append(swapped(out, "sp", k))
    return call(
        functools.partial(mix_kernel, sp_count - 1),
        shape(cols, bf16),
        [place, routes, route_weight, base, *returned],
    )


def shards(
    residual,
    queries,
    keys,
    values,
    segments,
    routes,
    route_weight,
    sinks,
    out_weight,
    norm_gain,
    expert_gate,
    expert_up,
    expert_down,
    shared_gate,
    shared_up,
    shared_down,
):
    rows_here = residual.shape[0]
    model_width = residual.shape[1]
    tp_count = lax.axis_size("tp")
    tp_index = lax.axis_index("tp")
    head_local = queries.shape[1] // HEAD_DIM
    kv_local = keys.shape[1] // HEAD_DIM
    group_size = head_local // kv_local
    window_len = WINDOW
    blocks = rows_here // window_len
    own_marks = (segments % 256 + 1).astype(jnp.bfloat16)
    prev_keys, prev_values, prev_marks = passed_along(
        (
            keys[rows_here - window_len :],
            values[rows_here - window_len :],
            own_marks[rows_here - window_len :],
        ),
        "sp",
        1,
    )
    key_band = banded(prev_keys, keys, window_len).reshape(
        blocks, 2 * window_len, kv_local, HEAD_DIM
    )
    value_band = banded(prev_values, values, window_len).reshape(
        blocks, 2 * window_len, kv_local, HEAD_DIM
    )
    mark_band = banded(prev_marks, own_marks, window_len).astype(jnp.float32)
    query_marks = own_marks.reshape(blocks, window_len).astype(jnp.float32)
    query_blocks = queries.reshape(blocks, window_len, kv_local, group_size, HEAD_DIM)
    scores = jnp.einsum(
        "nqhgd,nkhd->nhgqk", query_blocks, key_band, preferred_element_type=jnp.float32
    ) * HEAD_DIM ** (-0.5)
    offsets = jnp.arange(window_len)[:, None] + window_len - jnp.arange(2 * window_len)[None, :]
    allowed = (
        (offsets >= 0) & (offsets < window_len) & (query_marks[:, :, None] == mark_band[:, None, :])
    )
    sink_logits = sinks.reshape(kv_local, group_size)[None, :, :, None]
    masked = jnp.where(allowed[:, None, None], scores, -jnp.inf)
    top_score = jnp.maximum(jnp.max(masked, axis=-1), sink_logits)
    exp_terms = jnp.where(allowed[:, None, None], jnp.exp(scores - top_score[..., None]), 0.0)
    denominator = jnp.sum(exp_terms, axis=-1) + jnp.exp(sink_logits - top_score)
    probabilities = (exp_terms / denominator[..., None]).astype(jnp.bfloat16)
    attended = jnp.einsum(
        "nhgqk,nkhd->nqhgd", probabilities, value_band, preferred_element_type=jnp.float32
    )
    attended = attended.astype(jnp.bfloat16).reshape(rows_here, head_local * HEAD_DIM)
    partial_value = jnp.dot(attended, out_weight, preferred_element_type=jnp.float32)
    col_width = model_width // tp_count
    col_start = tp_index * col_width
    summed = lax.psum(partial_value, "tp")
    updated = (residual.astype(jnp.float32) + summed).astype(jnp.bfloat16)
    updated_f32 = updated.astype(jnp.float32)
    inv_rms = lax.rsqrt(jnp.mean(updated_f32 * updated_f32, axis=-1, keepdims=True) + epsilon)
    normed = (updated_f32 * inv_rms * norm_gain).astype(jnp.bfloat16)
    updated_cols = lax.dynamic_slice_in_dim(updated, col_start, col_width, 1)
    normed_cols = lax.dynamic_slice_in_dim(normed, col_start, col_width, 1)
    shared_pre = jnp.dot(normed, shared_gate, preferred_element_type=jnp.float32)
    shared_lin = jnp.dot(normed, shared_up, preferred_element_type=jnp.float32)
    shared_act = (jax.nn.silu(shared_pre) * shared_lin).astype(jnp.bfloat16)
    top_count = routes.shape[1]
    experts = lax.axis_size("sp")
    capacity = 2 * rows_here * top_count // experts
    flat_ids = routes.reshape(-1)
    one_hot = (flat_ids[:, None] == jnp.arange(experts, dtype=jnp.int32)[None, :]).astype(jnp.int32)
    rank_in = jnp.cumsum(one_hot, axis=0) - one_hot
    slot_dest = flat_ids * capacity + jnp.sum(rank_in * one_hot, axis=1)
    token_of = jnp.arange(rows_here * top_count, dtype=jnp.int32) // top_count
    slot_token = jnp.full((experts * capacity,), -1, jnp.int32).at[slot_dest].set(token_of)
    filled = slot_token >= 0
    safe_token = jnp.where(filled, slot_token, 0)
    outgoing = jnp.where(filled[:, None], normed_cols[safe_token], jnp.zeros((), jnp.bfloat16))
    pieces = lax.all_to_all(
        outgoing.reshape(experts, capacity, col_width),
        "sp",
        split_axis=0,
        concat_axis=0,
        tiled=True,
    )
    arrived = lax.all_gather(pieces, "tp", axis=2, tiled=True)
    expert_rows = arrived.reshape(-1, model_width)
    gate_pre = jnp.dot(expert_rows, expert_gate[0], preferred_element_type=jnp.float32)
    up_lin = jnp.dot(expert_rows, expert_up[0], preferred_element_type=jnp.float32)
    expert_act = (jax.nn.silu(gate_pre) * up_lin).astype(jnp.bfloat16)
    gathered_expert, gathered_shared = (
        lax.all_gather(expert_act, "tp", axis=1, tiled=True),
        lax.all_gather(shared_act, "tp", axis=1, tiled=True),
    )
    expert_out = jnp.dot(
        gathered_expert, expert_down[0], preferred_element_type=jnp.float32
    ).astype(jnp.bfloat16)
    returned = lax.all_to_all(
        expert_out.reshape(experts, capacity, col_width),
        "sp",
        split_axis=0,
        concat_axis=0,
        tiled=True,
    )
    returned = returned.reshape(experts * capacity, col_width)
    picked = returned[slot_dest].astype(jnp.float32).reshape(rows_here, top_count, col_width)
    routed = jnp.sum(picked * route_weight[:, :, None], axis=1)
    shared_cols = jnp.dot(gathered_shared, shared_down, preferred_element_type=jnp.float32)
    return (updated_cols.astype(jnp.float32) + shared_cols + routed).astype(jnp.bfloat16)


def is_dense(rows_here, kv_width, top_count, sizes):
    experts, tp_count = sizes["sp"], sizes["tp"]
    dense = 2 * rows_here * top_count // experts >= rows_here
    even = experts & (experts - 1) == 0 and tp_count & (tp_count - 1) == 0
    return dense and even and kv_width // tp_count == WINDOW and rows_here % WINDOW == 0


def choose(*args):
    sizes = {axis: lax.axis_size(axis) for axis in ("sp", "tp")}
    dense = is_dense(args[0].shape[0], args[2].shape[1] * sizes["tp"], args[5].shape[1], sizes)
    return (dense_shards if dense else shards)(*args)


def solution(mesh):
    placed = (
        P(("grp", "sp"), None),
        P(("grp", "sp"), "tp"),
        P(("grp", "sp"), "tp"),
        P(("grp", "sp"), "tp"),
        P(("grp", "sp")),
        P(("grp", "sp"), None),
        P(("grp", "sp"), None),
        P("tp"),
        P("tp", None),
        P(),
        P("sp", None, "tp"),
        P("sp", None, "tp"),
        P("sp", None, "tp"),
        P(None, "tp"),
        P(None, "tp"),
        P(None, "tp"),
    )
    return jax.shard_map(
        choose, mesh=mesh, in_specs=placed, out_specs=P(("grp", "sp"), "tp"), check_vma=False
    )
```

```python
import functools

import jax
import jax.numpy as jnp
from jax import lax
from jax.experimental import pallas as pl
from jax.experimental.pallas import tpu as pltpu
from jax.sharding import PartitionSpec as P


HEAD_DIM = 64
WINDOW = 128


epsilon = 1e-06


def passed_along(value, axis, steps):
    count = lax.axis_size(axis)
    leading, last = (max(0, -steps), min(count, count - steps))
    return lax.ppermute(value, axis, [(source, source + steps) for source in range(leading, last)])


def banded(prev_rows, own_rows, window_len):
    blocks = own_rows.shape[0] // window_len
    joined = jnp.concatenate([prev_rows, own_rows], axis=0)
    shaped = joined.reshape((blocks + 1, window_len) + own_rows.shape[1:])
    return jnp.concatenate([shaped[:-1], shaped[1:]], axis=1)


KERNEL_VMEM = 16 * 2**20


def swapped(value, axis, bit):
    count = lax.axis_size(axis)
    return lax.ppermute(value, axis, [(source, source ^ bit) for source in range(count)])


def gathered(value, far=None):
    pieces = {0: value}
    bit = lax.axis_size("tp") // 2
    while bit:
        more = {}
        for known, held in pieces.items():
            j = known ^ bit
            more[j] = swapped(held, "tp", bit) if far is None or known else far
        pieces.update(more)
        far = None
        bit //= 2
    return [pieces[j] for j in range(len(pieces))]


def dot32(left, right):
    return jnp.dot(left, right, preferred_element_type=jnp.float32)


def own_columns(ref, spot, width):
    return ref.at[:, pl.ds(pl.multiple_of(spot * width, width), width)]


def copy_all(sources, targets, sems):
    copies = [
        pltpu.make_async_copy(source, target, sems.at[n])
        for n, (source, target) in enumerate(zip(sources, targets, strict=True))
    ]
    for copy in copies:
        copy.start()
    for copy in copies:
        copy.wait()


def column(row):
    return jnp.transpose(jnp.broadcast_to(row, (8, row.shape[1])))[:, :1]


def prologue_kernel(marks_hbm, k_hbm, v_hbm, weight_hbm, packed_ref, row_ref, *refs):
    part_refs, sems = refs[:-1], refs[-1]
    span, rows = WINDOW, k_hbm.shape[0]
    place = lax.axis_index("tp")
    tail = slice(rows - span, rows)
    parts = [own_columns(weight_hbm, place ^ j, part.shape[1]) for j, part in enumerate(part_refs, 1)]
    copy_all(
        [marks_hbm, k_hbm.at[tail], v_hbm.at[tail], *parts],
        [row_ref, packed_ref.at[:span], packed_ref.at[span : 2 * span], *part_refs],
        sems,
    )
    marks = jnp.bitwise_and(row_ref[:, tail], 255) + 1
    marks = jnp.broadcast_to(marks.astype(jnp.float32), (packed_ref.shape[0] - 2 * span, span))
    packed_ref[2 * span :, :] = marks.astype(jnp.bfloat16)


def fetch_kernel(count, sliced, *refs):
    sources, targets, sems = refs[:count], refs[count:-1], refs[-1]
    place = lax.axis_index("tp")
    cut = [own_columns(source, place, target.shape[1]) for source, target in zip(sources[:sliced], targets)]
    copy_all([*cut, *sources[sliced:]], targets, sems)


def attend_kernel(sink_hbm, row_ref, q_ref, k_ref, v_ref, halo_ref, out_ref, sink_ref, sem):
    copy = pltpu.make_async_copy(sink_hbm, sink_ref, sem)
    copy.start()
    span = WINDOW
    rows = q_ref.shape[0]
    kv_local = k_ref.shape[1] // HEAD_DIM
    group_size = q_ref.shape[1] // k_ref.shape[1]
    halo = halo_ref[...]
    keys = jnp.concatenate([halo[:span], k_ref[...]], axis=0)
    values = jnp.concatenate([halo[span : 2 * span], v_ref[...]], axis=0)
    own = (jnp.bitwise_and(row_ref[...], 255) + 1).astype(jnp.float32)
    marks = jnp.concatenate([halo[2 * span : 2 * span + 1].astype(jnp.float32), own], axis=1)
    down_marks = column(own)
    place = lax.broadcasted_iota(jnp.int32, (span, 2 * span), 0)
    offsets = place + span - lax.broadcasted_iota(jnp.int32, (span, 2 * span), 1)
    near = (offsets >= 0) & (offsets < span)
    copy.wait()
    for block in range(rows // span):
        low = block * span
        allowed = near & (down_marks[low : low + span] == marks[:, low : low + 2 * span])
        outs = []
        for kv in range(kv_local):
            lanes = slice(kv * HEAD_DIM, (kv + 1) * HEAD_DIM)
            key_part = keys[low : low + 2 * span, lanes]
            value_part = values[low : low + 2 * span, lanes]
            for member in range(group_size):
                head = kv * group_size + member
                query = q_ref[low : low + span, head * HEAD_DIM : (head + 1) * HEAD_DIM]
                scores = lax.dot_general(
                    query, key_part, (((1,), (1,)), ((), ())), preferred_element_type=jnp.float32
                ) * HEAD_DIM ** (-0.5)
                sink = sink_ref[head]
                masked = jnp.where(allowed, scores, -jnp.inf)
                top = jnp.maximum(jnp.max(masked, axis=1, keepdims=True), sink)
                terms = jnp.exp(masked - top)
                total = jnp.sum(terms, axis=1, keepdims=True) + jnp.exp(sink - top)
                probs = (terms / total).astype(jnp.bfloat16)
                outs.append(dot32(probs, value_part).astype(jnp.bfloat16))
        out_ref[low : low + span, :] = jnp.concatenate(outs, axis=1)


def update_kernel(count, residual_ref, *refs):
    total = residual_ref[...].astype(jnp.float32)
    for j in range(count):
        total = total + dot32(refs[j][...], refs[count + j][...])
    refs[-1][...] = total.astype(jnp.bfloat16)


def hidden_kernel(count, pairs, gain_ref, *refs):
    pieces, weights, out_ref = refs[:count], refs[count:-1], refs[-1]
    place = lax.axis_index("tp")
    width = sum(piece.shape[1] for piece in pieces)
    hidden = weights[0].shape[2]
    squares = 0.0
    for piece in pieces:
        rows = piece[...].astype(jnp.float32)
        squares = squares + jnp.sum(rows * rows, axis=1, keepdims=True)
    scale = lax.rsqrt(squares / width + epsilon)
    sums = [None] * (2 * pairs)
    for j in range(count):
        at = place ^ j
        normed = (pieces[j][...].astype(jnp.float32) * scale * gain_ref[at]).astype(jnp.bfloat16)
        for n in range(2 * pairs):
            term = dot32(normed, weights[n][at])
            sums[n] = term if j == 0 else sums[n] + term
    for n in range(pairs):
        gate, lin = sums[2 * n], sums[2 * n + 1]
        act = gate / (1.0 + jnp.exp(-gate)) * lin
        out_ref[:, n * hidden : (n + 1) * hidden] = act.astype(jnp.bfloat16)


def down_kernel(count, down_ref, *refs):
    place = lax.axis_index("tp")
    total = dot32(refs[0][...], down_ref[place])
    for j in range(1, count):
        total = total + dot32(refs[j][...], down_ref[place ^ j])
    refs[-1][...] = total.astype(jnp.bfloat16)


def weights_of(routes_ref, weight_ref, steps):
    routes, weight, spot = routes_ref[...], weight_ref[...], lax.axis_index("sp")
    rows = []
    for k in range(steps):
        named = jnp.where(routes == (spot ^ k), weight, 0.0)
        rows.append(jnp.sum(named, axis=0, keepdims=True))
    rows += [jnp.zeros_like(rows[0])] * (-steps % 8)
    return jnp.transpose(jnp.concatenate(rows, axis=0))


def own_kernel(count, routes_ref, weight_ref, down_ref, shared_ref, updated_ref, *refs):
    place = lax.axis_index("tp")
    hidden = down_ref.shape[1]
    for j in range(count):
        terms = [
            dot32(refs[j][:, :hidden], down_ref[place ^ j]),
            dot32(refs[j][:, hidden:], shared_ref[place ^ j]),
        ]
        sums = terms if j == 0 else [old + term for old, term in zip(sums, terms, strict=True)]
    weight = weights_of(routes_ref, weight_ref, 1)[:, :1]
    routed = sums[0].astype(jnp.bfloat16).astype(jnp.float32)
    refs[-1][...] = updated_ref[...].astype(jnp.float32) + sums[1] + routed * weight


def mix_kernel(count, routes_ref, weight_ref, base_ref, *refs):
    weights = weights_of(routes_ref, weight_ref, count + 1)
    total = base_ref[...]
    for k in range(count):
        total = total + refs[k][...].astype(jnp.float32) * weights[:, k + 1 : k + 2]
    refs[-1][...] = total.astype(jnp.bfloat16)


def call(kernel, out, args, scalars=None):
    vmem = pl.BlockSpec(memory_space=pltpu.VMEM)
    specs, scratch = [vmem] * len(args), []
    if scalars is not None:
        args = [pltpu.with_memory_space_constraint(scalars, pltpu.HBM), *args]
        specs = [pl.BlockSpec(memory_space=pltpu.HBM), *specs]
        scratch = [pltpu.SMEM(scalars.shape, scalars.dtype), pltpu.SemaphoreType.DMA]
    return pl.pallas_call(
        kernel,
        out_shape=out,
        in_specs=specs,
        out_specs=vmem,
        scratch_shapes=scratch,
        compiler_params=pltpu.CompilerParams(vmem_limit_bytes=KERNEL_VMEM),
    )(*args)


def copier(kernel, outs, args, extra=0):
    args = [pltpu.with_memory_space_constraint(arg, pltpu.HBM) for arg in args]
    return pl.pallas_call(
        kernel,
        out_shape=[pltpu.VMEM(shape, dtype) for shape, dtype in outs],
        in_specs=[pl.BlockSpec(memory_space=pltpu.HBM)] * len(args),
        out_specs=[pl.BlockSpec(memory_space=pltpu.VMEM)] * len(outs),
        scratch_shapes=[pltpu.SemaphoreType.DMA((len(outs) + extra,))],
        compiler_params=pltpu.CompilerParams(vmem_limit_bytes=KERNEL_VMEM),
    )(*args)


def fetched(args, width=0, sliced=0):
    outs = [(arg.shape[:1] + (width,) if n < sliced else arg.shape, arg.dtype) for n, arg in enumerate(args)]
    return copier(functools.partial(fetch_kernel, len(args), sliced), outs, args)


def dense_shards(*args):
    return dense_steps(*args)


def dense_steps(
    residual,
    queries,
    keys,
    values,
    segments,
    routes,
    route_weight,
    sinks,
    out_weight,
    norm_gain,
    expert_gate,
    expert_up,
    expert_down,
    shared_gate,
    shared_up,
    shared_down,
):
    rows_here, model_width = residual.shape
    tp_count, sp_count = lax.axis_size("tp"), lax.axis_size("sp")
    span = WINDOW
    col_width = model_width // tp_count
    heads_width = out_weight.shape[0]
    bf16, f32 = jnp.bfloat16, jnp.float32
    shape = jax.ShapeDtypeStruct
    segments = segments[None, :]

    packed, _, *parts = copier(
        prologue_kernel,
        [((2 * span + 16, span), bf16), (segments.shape, segments.dtype)]
        + [((heads_width, col_width), bf16)] * (tp_count - 1),
        [segments, keys, values, out_weight],
        1,
    )
    halo = passed_along(packed, "sp", 1)
    parts = [swapped(part, "tp", j) for j, part in enumerate(parts, 1)]
    residual_cols, own_part, marks, own_queries, own_keys, own_values = fetched(
        [residual, out_weight, segments, queries, keys, values], col_width, 2
    )
    attended = call(attend_kernel, shape(queries.shape, bf16), [marks, own_queries, own_keys, own_values, halo], sinks)

    gain = norm_gain.reshape(tp_count, 1, col_width)
    gate, up, common_gate, common_up = [
        weight.reshape(tp_count, col_width, -1) for weight in (expert_gate, expert_up, shared_gate, shared_up)
    ]
    hidden = gate.shape[2]
    down, common_down = [weight.reshape(tp_count, hidden, col_width) for weight in (expert_down, shared_down)]
    gain, gate, up, common_gate, common_up, down, common_down, routes, route_weight = fetched(
        [gain, gate, up, common_gate, common_up, down, common_down, routes.T, route_weight.T]
    )
    own = call(
        functools.partial(update_kernel, tp_count),
        shape((rows_here, col_width), bf16),
        [residual_cols, *gathered(attended), own_part, *parts],
    )
    cols = (rows_here, col_width)

    last, half = sp_count - 1, tp_count // 2
    blocks = [gathered(own)]
    for k in range(1, last):
        blocks.append(gathered(swapped(own, "sp", k)))
    near, far = [swapped(blocks[last ^ 1][j], "sp", 1) for j in (0, half)]
    blocks.append(gathered(near, far))
    returned = []
    base = None
    for k in range(sp_count):
        pieces = blocks[k]
        pairs = 2 if k == 0 else 1
        weights = [gate, up, common_gate, common_up][: 2 * pairs]
        act = call(
            functools.partial(hidden_kernel, tp_count, pairs),
            shape((rows_here, pairs * hidden), bf16),
            [gain, *pieces, *weights],
        )
        acts = gathered(act)
        if k == 0:
            base = call(
                functools.partial(own_kernel, tp_count),
                shape(cols, f32),
                [routes, route_weight, down, common_down, own, *acts],
            )
        else:
            out = call(functools.partial(down_kernel, tp_count), shape(cols, bf16), [down, *acts])
            returned.append(swapped(out, "sp", k))
    return call(functools.partial(mix_kernel, sp_count - 1), shape(cols, bf16), [routes, route_weight, base, *returned])


def shards(
    residual,
    queries,
    keys,
    values,
    segments,
    routes,
    route_weight,
    sinks,
    out_weight,
    norm_gain,
    expert_gate,
    expert_up,
    expert_down,
    shared_gate,
    shared_up,
    shared_down,
):
    rows_here = residual.shape[0]
    model_width = residual.shape[1]
    tp_count = lax.axis_size("tp")
    tp_index = lax.axis_index("tp")
    head_local = queries.shape[1] // HEAD_DIM
    kv_local = keys.shape[1] // HEAD_DIM
    group_size = head_local // kv_local
    window_len = WINDOW
    blocks = rows_here // window_len
    own_marks = (segments % 256 + 1).astype(jnp.bfloat16)
    prev_keys, prev_values, prev_marks = passed_along(
        (
            keys[rows_here - window_len :],
            values[rows_here - window_len :],
            own_marks[rows_here - window_len :],
        ),
        "sp",
        1,
    )
    key_band = banded(prev_keys, keys, window_len).reshape(
        blocks, 2 * window_len, kv_local, HEAD_DIM
    )
    value_band = banded(prev_values, values, window_len).reshape(
        blocks, 2 * window_len, kv_local, HEAD_DIM
    )
    mark_band = banded(prev_marks, own_marks, window_len).astype(jnp.float32)
    query_marks = own_marks.reshape(blocks, window_len).astype(jnp.float32)
    query_blocks = queries.reshape(blocks, window_len, kv_local, group_size, HEAD_DIM)
    scores = jnp.einsum(
        "nqhgd,nkhd->nhgqk", query_blocks, key_band, preferred_element_type=jnp.float32
    ) * HEAD_DIM ** (-0.5)
    offsets = jnp.arange(window_len)[:, None] + window_len - jnp.arange(2 * window_len)[None, :]
    allowed = (
        (offsets >= 0) & (offsets < window_len) & (query_marks[:, :, None] == mark_band[:, None, :])
    )
    sink_logits = sinks.reshape(kv_local, group_size)[None, :, :, None]
    masked = jnp.where(allowed[:, None, None], scores, -jnp.inf)
    top_score = jnp.maximum(jnp.max(masked, axis=-1), sink_logits)
    exp_terms = jnp.where(allowed[:, None, None], jnp.exp(scores - top_score[..., None]), 0.0)
    denominator = jnp.sum(exp_terms, axis=-1) + jnp.exp(sink_logits - top_score)
    probabilities = (exp_terms / denominator[..., None]).astype(jnp.bfloat16)
    attended = jnp.einsum(
        "nhgqk,nkhd->nqhgd", probabilities, value_band, preferred_element_type=jnp.float32
    )
    attended = attended.astype(jnp.bfloat16).reshape(rows_here, head_local * HEAD_DIM)
    partial_value = jnp.dot(attended, out_weight, preferred_element_type=jnp.float32)
    col_width = model_width // tp_count
    col_start = tp_index * col_width
    summed = lax.psum(partial_value, "tp")
    updated = (residual.astype(jnp.float32) + summed).astype(jnp.bfloat16)
    updated_f32 = updated.astype(jnp.float32)
    inv_rms = lax.rsqrt(jnp.mean(updated_f32 * updated_f32, axis=-1, keepdims=True) + epsilon)
    normed = (updated_f32 * inv_rms * norm_gain).astype(jnp.bfloat16)
    updated_cols = lax.dynamic_slice_in_dim(updated, col_start, col_width, 1)
    normed_cols = lax.dynamic_slice_in_dim(normed, col_start, col_width, 1)
    shared_pre = jnp.dot(normed, shared_gate, preferred_element_type=jnp.float32)
    shared_lin = jnp.dot(normed, shared_up, preferred_element_type=jnp.float32)
    shared_act = (jax.nn.silu(shared_pre) * shared_lin).astype(jnp.bfloat16)
    top_count = routes.shape[1]
    experts = lax.axis_size("sp")
    capacity = 2 * rows_here * top_count // experts
    flat_ids = routes.reshape(-1)
    one_hot = (flat_ids[:, None] == jnp.arange(experts, dtype=jnp.int32)[None, :]).astype(jnp.int32)
    rank_in = jnp.cumsum(one_hot, axis=0) - one_hot
    slot_dest = flat_ids * capacity + jnp.sum(rank_in * one_hot, axis=1)
    token_of = jnp.arange(rows_here * top_count, dtype=jnp.int32) // top_count
    slot_token = jnp.full((experts * capacity,), -1, jnp.int32).at[slot_dest].set(token_of)
    filled = slot_token >= 0
    safe_token = jnp.where(filled, slot_token, 0)
    outgoing = jnp.where(filled[:, None], normed_cols[safe_token], jnp.zeros((), jnp.bfloat16))
    pieces = lax.all_to_all(
        outgoing.reshape(experts, capacity, col_width),
        "sp",
        split_axis=0,
        concat_axis=0,
        tiled=True,
    )
    arrived = lax.all_gather(pieces, "tp", axis=2, tiled=True)
    expert_rows = arrived.reshape(-1, model_width)
    gate_pre = jnp.dot(expert_rows, expert_gate[0], preferred_element_type=jnp.float32)
    up_lin = jnp.dot(expert_rows, expert_up[0], preferred_element_type=jnp.float32)
    expert_act = (jax.nn.silu(gate_pre) * up_lin).astype(jnp.bfloat16)
    gathered_expert, gathered_shared = (
        lax.all_gather(expert_act, "tp", axis=1, tiled=True),
        lax.all_gather(shared_act, "tp", axis=1, tiled=True),
    )
    expert_out = jnp.dot(
        gathered_expert, expert_down[0], preferred_element_type=jnp.float32
    ).astype(jnp.bfloat16)
    returned = lax.all_to_all(
        expert_out.reshape(experts, capacity, col_width),
        "sp",
        split_axis=0,
        concat_axis=0,
        tiled=True,
    )
    returned = returned.reshape(experts * capacity, col_width)
    picked = returned[slot_dest].astype(jnp.float32).reshape(rows_here, top_count, col_width)
    routed = jnp.sum(picked * route_weight[:, :, None], axis=1)
    shared_cols = jnp.dot(gathered_shared, shared_down, preferred_element_type=jnp.float32)
    return (updated_cols.astype(jnp.float32) + shared_cols + routed).astype(jnp.bfloat16)


def is_dense(rows_here, kv_width, top_count, sizes):
    experts, tp_count = sizes["sp"], sizes["tp"]
    dense = 2 * rows_here * top_count // experts >= rows_here
    even = experts & (experts - 1) == 0 and tp_count & (tp_count - 1) == 0
    return dense and even and kv_width // tp_count == WINDOW and rows_here % WINDOW == 0


def choose(*args):
    sizes = {axis: lax.axis_size(axis) for axis in ("sp", "tp")}
    dense = is_dense(args[0].shape[0], args[2].shape[1] * sizes["tp"], args[5].shape[1], sizes)
    return (dense_shards if dense else shards)(*args)


def solution(mesh):
    placed = (
        P(("grp", "sp"), None),
        P(("grp", "sp"), "tp"),
        P(("grp", "sp"), "tp"),
        P(("grp", "sp"), "tp"),
        P(("grp", "sp")),
        P(("grp", "sp"), None),
        P(("grp", "sp"), None),
        P("tp"),
        P("tp", None),
        P(),
        P("sp", None, "tp"),
        P("sp", None, "tp"),
        P("sp", None, "tp"),
        P(None, "tp"),
        P(None, "tp"),
        P(None, "tp"),
    )
    return jax.shard_map(
        choose, mesh=mesh, in_specs=placed, out_specs=P(("grp", "sp"), "tp"), check_vma=False
    )
```
